32 devices in a mesh: sp: 4 (over z), tp: 4 (over y, x), dp: 2 (over core).
Axes of the slice: x: 2, y: 2, z: 4, core: 2. Of those that a mesh axis runs over, the one named last changes fastest.
Arguments:
- latent: bfloat16 [2, 1024, 2048], P('dp', ('sp', 'tp')), may hold values from -6 to 6
- condition: bfloat16 [2, 2048], P('dp', ('sp', 'tp')), may hold values from -6 to 6
- context: bfloat16 [2, 32, 2048], P('dp', 'sp'), may hold values from -6 to 6
- context_vector: bfloat16 [2048], P(('sp', 'tp')), may hold values from -6 to 6
- modulator: bfloat16 [2048, 6144], P(('sp', 'tp')), may hold values from -0.3125 to 0.3125
- norm_gain: float32 [2048], replicated, may hold values from 0.1 to 1.9
- query_weight: bfloat16 [2048, 512], P(None, 'tp'), may hold values from -4 to 4
- key_weight: bfloat16 [2048, 512], P(None, 'tp'), may hold values from -0.125 to 0.125
- value_weight: bfloat16 [2048, 512], P(None, 'tp'), may hold values from -0.125 to 0.125
- head_gain: float32 [128], replicated, may hold values from 0.1 to 1.9
- lambdas: float32 [4], P('tp'), may hold values from 0.3 to 0.8
- context_bias: float32 [4, 2], P('tp'), may hold values from 1.3 to 2.7
- out_weight: bfloat16 [512, 2048], P('tp'), may hold values from -0.25 to 0.25
Outputs:
- updated: bfloat16 [2, 1024, 2048], P('dp', ('sp', 'tp'))
The draws below stay inside these ranges and needn't reach their ends.
All inputs are finite; a program needn't handle non-finite values.
Results may differ from the reference program's by a relative error of at most 0.024.
Values may be sent and summed in bfloat16 or wider, within the bound.
A program may use at most 64 MiB of HBM per device.

```python
import math
import jax
import jax.numpy as jnp
from jax import lax

D = 2048
HEADS = 4
HEAD = 64
SEQ = 1024
CTX = 32
SAMPLES = 2


def query_key_pair(key):
    key_spread = (1.5 * D) ** (-0.5)
    query_spread = (3.0 * D) ** (-0.5)
    key_part = key_spread * jax.random.normal(jax.random.fold_in(key, 11), (D, HEADS, 2, HEAD), jnp.float32)
    key_part = jnp.clip(key_part, -0.12, 0.12)
    query_part = query_spread * jax.random.normal(jax.random.fold_in(key, 12), (D, HEADS, 2, HEAD), jnp.float32)
    query_part = jnp.clip(query_part, -4.0, 4.0)
    return (query_part.reshape(D, HEADS * 2 * HEAD), key_part.reshape(D, HEADS * 2 * HEAD))


def draw_query_weight(key, part):
    return query_key_pair(key)[0].astype(jnp.bfloat16)


def draw_key_weight(key, part):
    return query_key_pair(key)[1].astype(jnp.bfloat16)


def steps_of(rng, extent, split, least, high):
    def one(dim, parts):
        heights = jax.random.uniform(jax.random.fold_in(jax.random.fold_in(rng, 6), dim), (parts,), jnp.float32, least / len(split), high / len(split))
        return jnp.repeat(jnp.exp(heights), extent[dim] // parts).reshape((-1,) + (1,) * (len(extent) - dim - 1))

    level = one(*split[0])
    for cut in split[1:]:
        level = level * one(*cut)
    return level


def noise(stream_key, dims, width, reach, shards=(), kind=jnp.bfloat16):
    result = jax.random.normal(stream_key, dims, jnp.float32) * width
    if len(shards) > 0:
        result = steps_of(stream_key, dims, shards, -0.22, 0.18) * result
    return jnp.clip(result, min=-reach, max=reach).astype(kind)


def setup_inputs(seed: int = 0) -> dict:
    key_of = jax.random.split(jax.random.key(seed), 14)
    return {
        "latent": noise(key_of[0], (SAMPLES, SEQ, D), 1.0, 6.0, ((0, 2), (1, 16))),
        "condition": noise(key_of[1], (SAMPLES, D), 1.0, 6.0, ((0, 2), (1, 16))),
        "context": noise(key_of[2], (SAMPLES, CTX, D), 1.0, 6.0, ((0, 2), (1, 4))),
        "context_vector": noise(key_of[3], (D,), 1.0, 6.0, ((0, 16),)),
        "modulator": noise(key_of[4], (D, 3 * D), (D // 6) ** -0.5, 0.3125, ((0, 16),)),
        "norm_gain": jnp.clip(1.0 + 0.18 * jax.random.normal(key_of[5], (D,), jnp.float32), 0.1, 1.9),
        "query_weight": draw_query_weight(jax.random.fold_in(key_of[13], 71), 0),
        "key_weight": draw_key_weight(jax.random.fold_in(key_of[13], 71), 0),
        "value_weight": noise(key_of[8], (D, 2 * HEAD * HEADS), D ** -0.5, 0.125, ((1, 4),)),
        "head_gain": jnp.clip(1.0 + 0.18 * jax.random.normal(key_of[9], (2 * HEAD,), jnp.float32), 0.1, 1.9),
        "lambdas": jnp.clip(0.3 + 0.5 * jax.random.uniform(key_of[10], (HEADS,), jnp.float32) ** steps_of(key_of[10], (HEADS,), ((0, 4),), -0.2, 0.2), 0.3, 0.8),
        "context_bias": jnp.clip(1.3 + 1.4000001 * jax.random.uniform(key_of[11], (HEADS, 2), jnp.float32) ** steps_of(key_of[11], (HEADS, 2), ((0, 4),), -0.2, 0.2), 1.3, 2.7),
        "out_weight": noise(key_of[12], (2 * HEAD * HEADS, D), (2 * HEAD * HEADS) ** -0.5, 0.25, ((0, 4),)),
    }


EPSILON = 1e-06
OUT_SCALE = 0.8

def modulate(inputs, gain_vector, shift_vector, scale_vector):
    as_float = inputs.astype(jnp.float32)
    normed = as_float * lax.rsqrt(lax.optimization_barrier(jnp.mean(as_float * as_float, axis=-1, keepdims=True)) + EPSILON)
    return (normed * gain_vector * (1.0 + scale_vector) + shift_vector).astype(jnp.bfloat16)

def reference(latent, condition, context, context_vector, modulator, norm_gain, query_weight, key_weight, value_weight, head_gain, lambdas, context_bias, out_weight):
    activated = jax.nn.silu(jnp.concatenate([condition, context_vector[None, :]], axis=0).astype(jnp.float32))
    activated = activated.astype(jnp.bfloat16)
    modulations = jnp.dot(activated, modulator, preferred_element_type=jnp.float32)
    ctx_shift = modulations[SAMPLES, :D]
    ctx_scale = modulations[SAMPLES, D:2 * D]
    block_rows = math.gcd(SEQ, 512)
    key_flags = jnp.concatenate([jnp.zeros((SEQ,), jnp.float32), jnp.ones((CTX,), jnp.float32)])
    key_bias = context_bias[:, :, None, None] * key_flags
    results = []
    for sample_index in range(SAMPLES):
        shift_vector = modulations[sample_index, :D]
        scale_vector = modulations[sample_index, D:2 * D]
        gate_vector = modulations[sample_index, 2 * D:]
        hidden = modulate(latent[sample_index], norm_gain, shift_vector, scale_vector)
        ctx_hidden = modulate(context[sample_index], norm_gain, ctx_shift, ctx_scale)
        queries = jnp.dot(hidden, query_weight, preferred_element_type=jnp.float32).astype(jnp.bfloat16)
        queries = queries.reshape(SEQ, HEADS, 2, HEAD)
        all_keys = jnp.concatenate([jnp.dot(hidden, key_weight, preferred_element_type=jnp.float32).astype(jnp.bfloat16), jnp.dot(ctx_hidden, key_weight, preferred_element_type=jnp.float32).astype(jnp.bfloat16)], axis=0)
        all_values = jnp.concatenate([jnp.dot(hidden, value_weight, preferred_element_type=jnp.float32).astype(jnp.bfloat16), jnp.dot(ctx_hidden, value_weight, preferred_element_type=jnp.float32).astype(jnp.bfloat16)], axis=0)
        keys_float = all_keys.reshape(SEQ + CTX, HEADS, 2, HEAD).astype(jnp.float32)
        values_float = all_values.reshape(SEQ + CTX, HEADS, 2 * HEAD).astype(jnp.float32)

        def attend(query_block):
            scores = jnp.einsum('qhmd,khmd->hmqk', query_block.astype(jnp.float32), keys_float) * HEAD ** (-0.5)
            scores = scores + key_bias
            row_max = lax.optimization_barrier(jnp.max(scores, axis=-1, keepdims=True))
            weights = jnp.exp(scores - row_max)
            totals = lax.optimization_barrier(jnp.sum(weights, axis=-1))
            rounded = lax.optimization_barrier(weights.astype(jnp.bfloat16)).astype(jnp.float32)
            summed = jnp.einsum('hmqk,khe->hmqe', rounded, values_float)
            mixed = summed[:, 0] / totals[:, 0, :, None] - lambdas[:, None, None] * summed[:, 1] / totals[:, 1, :, None]
            normed = mixed * lax.rsqrt(lax.optimization_barrier(jnp.mean(mixed * mixed, axis=-1, keepdims=True)) + EPSILON) * head_gain * OUT_SCALE
            return jnp.transpose(normed, (1, 0, 2)).reshape(block_rows, HEADS * 2 * HEAD).astype(jnp.bfloat16)
        query_blocks = queries.reshape(SEQ // block_rows, block_rows, HEADS, 2, HEAD)
        attended = lax.map(attend, query_blocks).reshape(SEQ, HEADS * 2 * HEAD)
        branch = jnp.dot(attended, out_weight, preferred_element_type=jnp.float32)
        results.append((latent[sample_index].astype(jnp.float32) + gate_vector * branch).astype(jnp.bfloat16))
    return jnp.stack(results)
```

```python
import functools

import jax
import jax.numpy as jnp
from jax import lax
from jax.experimental import pallas as pl
from jax.experimental.pallas import tpu as pltpu
from jax.sharding import PartitionSpec as P

EPSILON = 1e-06
OUT_SCALE = 0.8
KEY_BLOCK = 2048
LOW_START = -1e30


def modulate(inputs, gain_vector, shift_vector, scale_vector):
    as_float = inputs.astype(jnp.float32)
    normed = as_float * lax.rsqrt(jnp.mean(as_float * as_float, axis=-1, keepdims=True) + EPSILON)
    return (normed * gain_vector * (1.0 + scale_vector) + shift_vector).astype(jnp.bfloat16)


def fold_block(running, queries, keys_in, values_in, key_flags, bias_table, score_scale):
    run_max, run_total, summed = running
    scores = (
        jnp.einsum("qhmd,khmd->hmqk", queries, keys_in, preferred_element_type=jnp.float32)
        * score_scale
    )
    if key_flags is not None:
        scores = scores + bias_table[:, :, None, None] * key_flags
    new_max = jnp.maximum(run_max, jnp.max(scores, axis=-1))
    shrink = jnp.exp(run_max - new_max)
    weights = jnp.exp(scores - new_max[..., None])
    run_total = run_total * shrink + jnp.sum(weights, axis=-1)
    summed = summed * shrink[..., None] + jnp.einsum(
        "hmqk,khe->hmqe",
        weights.astype(jnp.bfloat16),
        values_in,
        preferred_element_type=jnp.float32,
    )
    return (new_max, run_total, summed)


def fold_keys(running, queries, keys_in, values_in, key_flags, bias_table, score_scale):
    full_blocks = keys_in.shape[0] // KEY_BLOCK
    if full_blocks > 1:
        edge = full_blocks * KEY_BLOCK
        stacked = (
            keys_in[:edge].reshape((full_blocks, KEY_BLOCK) + keys_in.shape[1:]),
            values_in[:edge].reshape((full_blocks, KEY_BLOCK) + values_in.shape[1:]),
        )
        if key_flags is not None:
            stacked = stacked + (key_flags[:edge].reshape(full_blocks, KEY_BLOCK),)

        def fold_step(current, block_data):
            flag_part = None if key_flags is None else block_data[2]
            return (
                fold_block(
                    current,
                    queries,
                    block_data[0],
                    block_data[1],
                    flag_part,
                    bias_table,
                    score_scale,
                ),
                None,
            )

        running, ignored = lax.scan(fold_step, running, stacked)
        keys_in = keys_in[edge:]
        values_in = values_in[edge:]
        key_flags = None if key_flags is None else key_flags[edge:]
    if keys_in.shape[0] > 0:
        running = fold_block(
            running, queries, keys_in, values_in, key_flags, bias_table, score_scale
        )
    return running


def body(
    latent,
    condition,
    context,
    context_vector,
    modulator,
    norm_gain,
    query_weight,
    key_weight,
    value_weight,
    head_gain,
    lambdas,
    context_bias,
    out_weight,
):
    model_width = latent.shape[2]
    local_heads = lambdas.shape[0]
    query_width = query_weight.shape[1]
    head_size = query_width // (2 * local_heads)
    value_size = value_weight.shape[1] // local_heads
    score_scale = head_size ** (-0.5)
    activated = jax.nn.silu(
        jnp.concatenate([condition, context_vector[None, :]], axis=0).astype(jnp.float32)
    )
    partial_terms = jnp.dot(
        activated.astype(jnp.bfloat16), modulator, preferred_element_type=jnp.float32
    )
    modulations = lax.psum(partial_terms, ("sp", "tp"))
    hidden = modulate(
        latent[0],
        norm_gain,
        modulations[0, :model_width],
        modulations[0, model_width : 2 * model_width],
    )
    ctx_hidden = modulate(
        context[0],
        norm_gain,
        modulations[1, :model_width],
        modulations[1, model_width : 2 * model_width],
    )
    gate_vector = modulations[0, 2 * model_width :]
    incoming = lax.all_gather(hidden, "tp", axis=0, tiled=True)
    projected = jnp.concatenate(
        [
            jnp.dot(incoming, query_weight, preferred_element_type=jnp.float32),
            jnp.dot(incoming, key_weight, preferred_element_type=jnp.float32),
            jnp.dot(incoming, value_weight, preferred_element_type=jnp.float32),
        ],
        axis=1,
    ).astype(jnp.bfloat16)
    query_rows = projected.shape[0]
    queries = projected[:, :query_width].reshape(query_rows, local_heads, 2, head_size)
    own_keys = projected[:, query_width : 2 * query_width]
    own_values = projected[:, 2 * query_width :]
    gathered_context = lax.all_gather(ctx_hidden, "sp", axis=0, tiled=True)
    ctx_keys = jnp.dot(gathered_context, key_weight, preferred_element_type=jnp.float32).astype(
        jnp.bfloat16
    )
    ctx_values = jnp.dot(gathered_context, value_weight, preferred_element_type=jnp.float32).astype(
        jnp.bfloat16
    )
    start_carry = (
        jnp.full((local_heads, 2, query_rows), LOW_START, jnp.float32),
        jnp.zeros((local_heads, 2, query_rows), jnp.float32),
        jnp.zeros((local_heads, 2, query_rows, value_size), jnp.float32),
    )
    pieces = (own_keys, own_values)
    initial = fold_keys(
        start_carry,
        queries,
        ctx_keys.reshape(-1, local_heads, 2, head_size),
        ctx_values.reshape(-1, local_heads, value_size),
        jnp.ones((ctx_keys.shape[0],), jnp.float32),
        context_bias,
        score_scale,
    )
    incoming = (
        lax.all_gather(pieces[0], "sp", axis=0, tiled=True),
        lax.all_gather(pieces[1], "sp", axis=0, tiled=True),
    )
    run_max, run_total, summed = fold_keys(
        initial,
        queries,
        incoming[0].reshape(-1, local_heads, 2, head_size),
        incoming[1].reshape(-1, local_heads, value_size),
        None,
        context_bias,
        score_scale,
    )
    mixed = (
        summed[:, 0] / run_total[:, 0, :, None]
        - lambdas[:, None, None] * summed[:, 1] / run_total[:, 1, :, None]
    )
    normed = (
        mixed
        * lax.rsqrt(jnp.mean(mixed * mixed, axis=-1, keepdims=True) + EPSILON)
        * head_gain
        * OUT_SCALE
    )
    attended = (
        jnp.transpose(normed, (1, 0, 2))
        .reshape(query_rows, local_heads * value_size)
        .astype(jnp.bfloat16)
    )
    exchanged = lax.all_to_all(attended, "tp", split_axis=0, concat_axis=1, tiled=True)
    whole_weight = lax.all_gather(out_weight, "tp", axis=0, tiled=True)
    branch = jnp.dot(exchanged, whole_weight, preferred_element_type=jnp.float32)
    result = (latent[0].astype(jnp.float32) + gate_vector * branch).astype(jnp.bfloat16)
    return result[None]


MESH = pl.DeviceIdType.MESH
LANES = 128


class Phases:
    def __init__(self):
        self.open = None

    def __call__(self, name):
        if self.open is not None:
            self.open.__exit__(None, None, None)
        self.open = None
        if name is not None:
            self.open = jax.named_scope(name)
            self.open.__enter__()


def fused_kernel(
    sp_n, tp_n, score_scale,
    latent, condition_in, context, vector_in, modulator, gain_in,
    query_weight, key_weight, value_weight, head_gain_in, lambdas_in, bias_in, out_weight,
    out,
    condition, context_vector, norm_gain, head_gain, lambdas, context_bias,
    mod_v, gate_v, fast_p, fast_z, slow_z, slow_p, lat, ctx, w_qkv, w_out, vecs, hid, kvb, ckv,
    att_out, att_in, acc,
    small_sem, own_sem, mod_sem, two_sem, far_sem, fp_ss, fp_rs, fz_ss, fz_rs, sz_ss, sz_rs, sl_ss, sl_rs,
    lat_ss, lat_rs, ck_ss, ck_rs, kv_ss, kv_rs, wt_ss, wt_rs, wd_ss, wd_rs, at_ss, at_rs,
):
    sp = lax.axis_index("sp")
    tp = lax.axis_index("tp")
    dp = lax.axis_index("dp")
    across = tp + 1 - 2 * lax.rem(tp, 2)
    along = lax.rem(tp + 2, 4)
    corner = along + 1 - 2 * lax.rem(along, 2)
    roles = (tp, across, along, corner)
    half = lat.shape[1]
    width = lat.shape[2]
    rows = half * 2
    qrows = rows * tp_n
    depth = gate_v.shape[0]
    ctx_rows = ctx.shape[0]
    high = (2 * sp) // sp_n

    def z_peer(t):
        up = (t - 1) + jnp.where(t - 1 >= sp, 1, 0)
        down = (sp_n - t) - jnp.where(sp_n - t <= sp, 1, 0)
        return jnp.where(high == 0, up, down)

    phase = Phases()
    phase("enter")
    barrier = pltpu.get_barrier_semaphore()

    def greet(where):
        pl.semaphore_signal(barrier, inc=1, device_id=where, device_id_type=MESH)

    has_up, has_down = sp + 1 < sp_n, sp > 0
    middle = jnp.logical_and(has_up, has_down)
    for peer in (across, along, corner):
        greet((sp, peer, dp))
    pl.when(has_up)(lambda: greet((sp + 1, tp, dp)))
    pl.when(has_down)(lambda: greet((sp - 1, tp, dp)))
    greet((sp, tp, 1 - dp))

    small = [
        pltpu.make_async_copy(source, place, small_sem.at[k])
        for k, (source, place) in enumerate((
            (condition_in, condition), (vector_in, context_vector), (context, ctx),
            (gain_in, norm_gain), (head_gain_in, head_gain), (lambdas_in, lambdas),
            (bias_in, context_bias),
        ))
    ]
    cut = width // MOD_CUTS

    def mod_loads(k):
        return [
            pltpu.make_async_copy(
                modulator.at[:, pl.ds(part * width + k * cut, cut)], mod_v.at[part, :, pl.ds(k * cut, cut)],
                mod_sem.at[k],
            )
            for part in range(2)
        ]

    def here(place, sem):
        return pltpu.make_async_copy(place, place, sem)

    loads = [
        pltpu.make_async_copy(latent, lat.at[pl.ds(tp * 2, 2)], own_sem.at[0]),
        pltpu.make_async_copy(modulator.at[:, pl.ds(2 * width, width)], gate_v, own_sem.at[1]),
        pltpu.make_async_copy(key_weight, w_qkv.at[:, pl.ds(0, LANES)], own_sem.at[2]),
        pltpu.make_async_copy(value_weight, w_qkv.at[:, pl.ds(LANES, LANES)], own_sem.at[2]),
        pltpu.make_async_copy(query_weight, w_qkv.at[:, pl.ds(2 * LANES, LANES)], own_sem.at[2]),
        pltpu.make_async_copy(out_weight, w_out.at[pl.ds(tp * 4, 4)], own_sem.at[3]),
    ]
    for load in small[:2]:
        load.start()
    for k in range(MOD_CUTS):
        for load in mod_loads(k):
            load.start()

    phase("partial")
    for load in small[:2]:
        load.wait()
    rows_in = jnp.concatenate([condition[...], context_vector[...]], axis=0).astype(jnp.float32)
    activated = jax.nn.silu(rows_in).astype(jnp.bfloat16)
    own_act, ctx_act = activated[0:1], activated[1:2]
    blank = jnp.zeros_like(own_act)
    left = jnp.concatenate([own_act, blank, ctx_act, blank], axis=0)
    right = jnp.concatenate([blank, own_act, blank, ctx_act], axis=0)
    stacked = jnp.concatenate([left, right], axis=1)
    for load in loads[:2] + small[2:] + loads[2:]:
        load.start()
    for k in range(MOD_CUTS):
        cols = slice(k * cut, (k + 1) * cut)
        here(mod_v.at[:, :, pl.ds(k * cut, cut)], mod_sem.at[k]).wait()
        terms = jnp.dot(
            stacked, mod_v[:, :, cols].reshape(2 * depth, cut), preferred_element_type=jnp.float32
        ).astype(jnp.bfloat16)
        fast_p[tp, :, cols] = terms[0:2]
        slow_z[sp, 0:2, cols] = terms[2:4]

    phase("barrier")
    pl.semaphore_wait(barrier, jnp.where(middle, 6, 5))

    def vouch(sem, where):
        pl.semaphore_signal(sem, inc=1, device_id=where, device_id_type=MESH)

    def vouch_both():
        vouch(two_sem, (sp + 1, tp, dp))
        vouch(two_sem, (sp - 1, tp, dp))

    pl.when(middle)(vouch_both)
    phase("sends")


    def plane_copy(buf, d, ss, rs):
        return pltpu.make_async_remote_copy(
            src_ref=buf.at[tp], dst_ref=buf.at[tp], send_sem=ss, recv_sem=rs,
            device_id=(sp, roles[d], dp), device_id_type=MESH,
        )

    def z_copy(buf, t, ss, rs):
        return pltpu.make_async_remote_copy(
            src_ref=buf.at[sp], dst_ref=buf.at[sp], send_sem=ss, recv_sem=rs,
            device_id=(z_peer(t), tp, dp), device_id_type=MESH,
        )

    def some(place, ss, rs):
        return pltpu.make_async_remote_copy(
            src_ref=place, dst_ref=place, send_sem=ss, recv_sem=rs,
            device_id=(sp, across, dp), device_id_type=MESH,
        )

    def three(buf, ss, rs):
        return some(buf.at[pl.ds(0, 3)], ss, rs)

    for d in (3, 1, 2):
        plane_copy(fast_p, d, fp_ss, fp_rs).start()
    phase("lat_first")

    class Plane:
        def __init__(self, buf, index, ss, rs):
            self.buf, self.index, self.ss, self.rs = buf, index, ss, rs

        def copy(self, owner, part_no, target, kind):
            place = self.buf.at[self.index(owner, part_no)]
            return pltpu.make_async_remote_copy(
                src_ref=place, dst_ref=place, send_sem=self.ss,
                recv_sem=self.rs.at[kind * 2 + part_no],
                device_id=(sp, target, dp), device_id_type=MESH,
            )

        def first(self):
            return [
                self.copy(tp, 0, across, 0),
                self.copy(tp, 1, along, 1),
                self.copy(tp, 1, across, 0),
                self.copy(tp, 0, along, 1),
            ]

        def relays(self):
            return [self.copy(across, 0, along, 2), self.copy(along, 1, across, 2)]

        def arrival(self, kind, part_no):
            owner = (across, along, corner)[kind]
            return self.copy(owner, part_no, across, kind)

    plane = Plane(lat, lambda o, q: o * 2 + q, lat_ss, lat_rs)
    loads[0].wait()
    for copy in plane.first():
        copy.start()

    loads[1].wait()
    gate_rows = jnp.concatenate([own_act, blank], axis=0)
    slow_z[sp, 2:4] = jnp.dot(gate_rows, gate_v[...], preferred_element_type=jnp.float32).astype(jnp.bfloat16)
    phase("slow_send")
    z_copy(slow_z, 1, sz_ss, sz_rs).start()
    pl.semaphore_wait(two_sem, 1)
    pl.when(middle)(lambda: vouch(far_sem, (jnp.where(high == 0, sp - 1, sp + 1), tp, dp)))
    z_copy(slow_z, 2, sz_ss, sz_rs).start()
    pl.when(jnp.logical_not(middle))(lambda: pl.semaphore_wait(far_sem, 1))
    z_copy(slow_z, 3, sz_ss, sz_rs).start()

    def row_scale(at):
        x = lat[at].astype(jnp.float32)
        return lax.rsqrt(jnp.mean(x * x, axis=-1, keepdims=True) + EPSILON)

    scales = {}

    def measure(role, q):
        scales[role, q] = row_scale(roles[role] * 2 + q)

    def total_of(buf, count):
        total = buf[0].astype(jnp.float32)
        for p in range(1, count):
            total = total + buf[p].astype(jnp.float32)
        return total

    for q in range(2):
        measure(0, q)
    phase("plane_wait")
    three(fast_p, fp_ss, fp_rs).wait_recv()
    fast_z[sp] = total_of(fast_p, tp_n).astype(jnp.bfloat16)
    for t in (3, 2, 1):
        z_copy(fast_z, t, fz_ss, fz_rs).start()

    phase("lat_relay")
    relays = plane.relays()
    plane.arrival(0, 0).wait_recv()
    relays[0].start()
    plane.arrival(1, 1).wait_recv()
    relays[1].start()
    measure(1, 0)
    measure(2, 1)
    phase("slow_relay")
    three(slow_z, sz_ss, sz_rs).wait_recv()
    slow_p[tp] = total_of(slow_z, sp_n).astype(jnp.bfloat16)
    for d in (3, 1, 2):
        plane_copy(slow_p, d, sl_ss, sl_rs).start()
    loads[5].wait()
    wplane = Plane(w_out, lambda o, q: o * 4 + dp * 2 + q, wt_ss, wt_rs)
    for copy in wplane.first():
        copy.start()
    for load in small[2:]:
        load.wait()
    here(w_qkv, own_sem.at[2]).wait()

    phase("z_wait")
    three(fast_z, fz_ss, fz_rs).wait_recv()
    fast = total_of(fast_z, sp_n)
    gain = norm_gain[...]
    vecs[0:1, :] = gain * (1.0 + fast[1:2])
    vecs[1:2, :] = fast[0:1]

    def norm_role(role):
        for q in range(2):
            at = (role * 2 + q) * half
            x = lat[roles[role] * 2 + q].astype(jnp.float32)
            hid[at : at + half, :] = (x * scales[role, q] * vecs[0:1, :] + vecs[1:2, :]).astype(jnp.bfloat16)

    def kv_copy(block, q, to):
        place = kvb.at[q * sp_n + block]
        spread = jnp.abs(to - block)
        end = jnp.logical_or(to == 0, to == sp_n - 1)
        far = jnp.logical_or(spread == sp_n - 1, jnp.logical_and(spread == 2, jnp.logical_not(end)))
        slot = RELAYED if q == RELAYED else jnp.where(far, q, RELAYED + 1)
        return pltpu.make_async_remote_copy(
            src_ref=place, dst_ref=place, send_sem=kv_ss, recv_sem=kv_rs.at[slot],
            device_id=(to, tp, dp), device_id_type=MESH,
        )

    def kv_wait(count, slot):
        return some(kvb.at[pl.ds(0, count)], kv_ss, kv_rs.at[slot])

    def kv_rows(first, last):
        product = jnp.dot(hid[first:last, :], w_qkv[:, : 2 * LANES], preferred_element_type=jnp.float32)
        return product.astype(jnp.bfloat16)

    def kv_send(q):
        far = kv_copy(sp, q, z_peer(3))
        if q < RELAYED:
            pl.when(middle)(far.start)
        else:
            far.start()
        for t in (2, 1):
            kv_copy(sp, q, z_peer(t)).start()

    def kv_role(q):
        kvb[q * sp_n + sp] = kv_rows(q * rows, (q + 1) * rows)
        kv_send(q)

    def relay(q):
        def act():
            kv_wait(1, q).wait_recv()
            kv_copy(z_peer(3), q, jnp.where(high == 0, sp - 1, sp + 1)).start()

        pl.when(middle)(act)

    phase("kv_own")
    norm_role(0)
    kv_role(0)
    phase("kv_across")
    plane.arrival(0, 1).wait_recv()
    measure(1, 1)
    norm_role(1)
    kv_role(1)
    phase("kv_along")
    plane.arrival(1, 0).wait_recv()
    measure(2, 0)
    norm_role(2)
    kv_role(2)
    phase("kv_corner")
    for q in range(2):
        plane.arrival(2, q).wait_recv()
        measure(3, q)
    norm_role(3)
    kv_role(3)

    phase("queries")
    queries = jnp.dot(hid[:qrows, :], w_qkv[:, 2 * LANES :], preferred_element_type=jnp.float32) * score_scale
    queries = queries.astype(jnp.bfloat16)
    head = queries.shape[1] // 2
    lane = lax.broadcasted_iota(jnp.int32, queries.shape, 1)
    zero = jnp.zeros_like(queries)
    both = jnp.concatenate(
        [jnp.where(lane < head, queries, zero), jnp.where(lane < head, zero, queries)], axis=0
    )

    def score(keys):
        return lax.dot_general(
            both, keys, (((1,), (1,)), ((), ())), preferred_element_type=jnp.float32
        )

    map_row = lax.broadcasted_iota(jnp.int32, (2 * qrows, 1), 0)
    bias = jnp.where(map_row < qrows, context_bias[0:1, 0:1], context_bias[0:1, 1:2])

    def fold(running, scores, values):
        top = jnp.max(scores, axis=-1, keepdims=True)
        if running is not None:
            top = jnp.maximum(running[0], top)
        weights = jnp.exp(scores - top)
        count = jnp.sum(weights, axis=-1, keepdims=True)
        summed = jnp.dot(weights.astype(jnp.bfloat16), values, preferred_element_type=jnp.float32)
        if running is not None:
            shrink = jnp.exp(running[0] - top)
            count = running[1] * shrink + count
            summed = running[2] * shrink + summed
        return top, count, summed

    def fold_keys_in(running, places):
        block = jnp.concatenate([kvb[place] for place in places], axis=0)
        return fold(running, score(block[:, :LANES]), block[:, LANES:])

    def piece(t, q):
        return q * sp_n + (sp if t == 0 else z_peer(t))

    phase("fold_own")
    running = fold_keys_in(None, [piece(0, q) for q in range(tp_n)])
    phase("slow_wait")
    three(slow_p, sl_ss, sl_rs).wait_recv()
    slow = total_of(slow_p, tp_n)
    vecs[2:3, :] = gain * (1.0 + slow[1:2])
    vecs[3:4, :] = slow[0:1]
    vecs[4:5, :] = slow[2:3]
    cx = ctx[...].astype(jnp.float32)
    cx = cx * lax.rsqrt(jnp.mean(cx * cx, axis=-1, keepdims=True) + EPSILON)
    hid[qrows : qrows + ctx_rows, :] = (cx * vecs[2:3, :] + vecs[3:4, :]).astype(jnp.bfloat16)
    ckv[sp] = kv_rows(qrows, qrows + ctx_rows)
    for t in (1, 2, 3):
        z_copy(ckv, t, ck_ss, ck_rs).start()
    phase("relays")
    for q in range(RELAYED):
        relay(q)

    def sibling(owner, part_no):
        place = w_out.at[owner * 4 + dp * 2 + part_no]
        return pltpu.make_async_remote_copy(
            src_ref=place, dst_ref=place, send_sem=wd_ss, recv_sem=wd_rs,
            device_id=(sp, tp, 1 - dp), device_id_type=MESH,
        )

    owners = (across, along, corner)

    def swap(kind, part_no, wait=True):
        if wait:
            wplane.arrival(kind, part_no).wait_recv()
        sibling(owners[kind], part_no).start()

    phase("w_relay")
    w_relays = wplane.relays()
    wplane.arrival(0, 0).wait_recv()
    w_relays[0].start()
    wplane.arrival(1, 1).wait_recv()
    w_relays[1].start()
    swap(0, 0, False)
    swap(1, 1, False)
    phase("take_near")
    kv_wait(2 * RELAYED, RELAYED + 1).wait_recv()
    phase("fold_near")
    running = fold_keys_in(running, [piece(t, q) for t in (1, 2) for q in range(RELAYED)])
    phase("ctx")
    three(ckv, ck_ss, ck_rs).wait_recv()
    ctx_kv = ckv[...].reshape(sp_n * ctx_rows, 2 * LANES)
    running = fold(running, score(ctx_kv[:, :LANES]) + bias, ctx_kv[:, LANES:])
    phase("w_second")
    swap(0, 1)
    swap(1, 0)
    phase("take_far")
    for q in range(RELAYED):
        pl.when(jnp.logical_not(middle))(kv_wait(1, q).wait_recv)
    running = fold_keys_in(running, [piece(3, q) for q in range(RELAYED)])
    phase("take_last")
    kv_wait(3, RELAYED).wait_recv()
    phase("fold_last")
    running = fold_keys_in(running, [piece(t, RELAYED) for t in (1, 2, 3)])

    phase("finish")
    top, count, summed = running
    shares = summed / count
    mixed = shares[:qrows] - lambdas[...] * shares[qrows:]
    normed = (
        mixed
        * lax.rsqrt(jnp.mean(mixed * mixed, axis=-1, keepdims=True) + EPSILON)
        * head_gain[...]
        * OUT_SCALE
    ).astype(jnp.bfloat16)
    for p in range(tp_n):
        att_out[p] = normed[p * rows : (p + 1) * rows]

    def at_copy(d):
        return pltpu.make_async_remote_copy(
            src_ref=att_out.at[d], dst_ref=att_in.at[tp], send_sem=at_ss, recv_sem=at_rs.at[d // 2],
            device_id=(sp, roles[d], dp), device_id_type=MESH,
        )

    for d in (3, 1, 2):
        at_copy(d).start()
    att_in[tp] = att_out[0]

    phase("w_wait")
    swap(2, 0)
    swap(2, 1)
    some(w_out.at[pl.ds(0, 6)], wd_ss, wd_rs).wait_recv()

    def pair_terms(base, cols):
        pair = jnp.concatenate([att_in[base], att_in[base + 1]], axis=1)
        weight = w_out[pl.ds(base * 4, 8), :, cols].reshape(pair.shape[1], cols.stop - cols.start)
        return jnp.dot(pair, weight, preferred_element_type=jnp.float32)

    step = 512
    spans = [slice(first, first + step) for first in range(0, width, step)]
    phase("at_wait")
    some(att_in.at[pl.ds(0, 1)], at_ss, at_rs.at[0]).wait_recv()
    for cols in spans:
        acc[:, cols] = pair_terms(tp - lax.rem(tp, 2), cols)
    phase("at_wait2")
    some(att_in.at[pl.ds(0, 2)], at_ss, at_rs.at[1]).wait_recv()

    phase("out")
    for cols in spans:
        branch = acc[:, cols] + pair_terms(along - lax.rem(along, 2), cols)
        for q in range(2):
            mine = lat[tp * 2 + q, :, cols].astype(jnp.float32)
            update = mine + vecs[4:5, cols] * branch[q * half : (q + 1) * half]
            out[q * half : (q + 1) * half, cols] = update.astype(jnp.bfloat16)

    phase("drain")
    for buf, ss, rs in (
        (fast_p, fp_ss, fp_rs), (fast_z, fz_ss, fz_rs), (slow_z, sz_ss, sz_rs), (slow_p, sl_ss, sl_rs),
        (ckv, ck_ss, ck_rs), (att_out, at_ss, at_rs.at[0]),
    ):
        three(buf, ss, rs).wait_send()
    some(lat.at[pl.ds(0, 6)], lat_ss, lat_rs.at[0]).wait_send()
    some(w_out.at[pl.ds(0, 6)], wt_ss, wt_rs.at[0]).wait_send()
    some(w_out.at[pl.ds(0, 6)], wd_ss, wd_rs).wait_send()
    pl.when(middle)(kv_wait(tp_n * 3 + RELAYED, 0).wait_send)
    pl.when(jnp.logical_not(middle))(kv_wait(tp_n * 3 - RELAYED, 0).wait_send)
    phase(None)


RELAYED = 3
MOD_CUTS = 4


def fused(
    axes, latent, condition, context, context_vector, modulator, norm_gain, query_weight,
    key_weight, value_weight, head_gain, lambdas, context_bias, out_weight,
):
    sp_n, tp_n, dp_n = axes
    rows, width = latent.shape[1:]
    half = rows // 2
    depth = modulator.shape[0]
    ctx_rows = context.shape[1]
    qw = query_weight.shape[1]
    value = value_weight.shape[1]
    qrows = rows * tp_n
    wrows = out_weight.shape[0] // 4
    bf, f32 = jnp.bfloat16, jnp.float32
    vm = pl.BlockSpec(memory_space=pltpu.VMEM)
    hb = pl.BlockSpec(memory_space=pltpu.HBM)
    dma = lambda k: pltpu.SemaphoreType.DMA((k,))
    result = pl.pallas_call(
        functools.partial(fused_kernel, sp_n, tp_n, (qw // 2) ** (-0.5)),
        out_shape=pltpu.VMEM((rows, width), bf),
        in_specs=[hb] * 13,
        out_specs=vm,
        scratch_shapes=[
            pltpu.VMEM(condition.shape, bf),
            pltpu.VMEM((1, context_vector.shape[0]), bf),
            pltpu.VMEM((1, width), f32),
            pltpu.VMEM((1, value), f32),
            pltpu.VMEM((1, 1), f32),
            pltpu.VMEM(context_bias.shape, f32),
            pltpu.VMEM((2, depth, width), bf),
            pltpu.VMEM((depth, width), bf),
            pltpu.VMEM((tp_n, 2, width), bf),
            pltpu.VMEM((sp_n, 2, width), bf),
            pltpu.VMEM((sp_n, 4, width), bf),
            pltpu.VMEM((tp_n, 4, width), bf),
            pltpu.VMEM((tp_n * 2, half, width), bf),
            pltpu.VMEM((ctx_rows, width), bf),
            pltpu.VMEM((width, 2 * qw + value), bf),
            pltpu.VMEM((tp_n * 4, wrows, width), bf),
            pltpu.VMEM((8, width), f32),
            pltpu.VMEM((qrows + ctx_rows, width), bf),
            pltpu.VMEM((sp_n * tp_n, rows, qw + value), bf),
            pltpu.VMEM((sp_n, ctx_rows, qw + value), bf),
            pltpu.VMEM((tp_n, rows, value), bf),
            pltpu.VMEM((tp_n, rows, value), bf),
            pltpu.VMEM((rows, width), f32),
            dma(7), dma(4), dma(MOD_CUTS), *[pltpu.SemaphoreType.REGULAR] * 2,
            *[pltpu.SemaphoreType.DMA] * 8, pltpu.SemaphoreType.DMA, dma(6), pltpu.SemaphoreType.DMA,
            pltpu.SemaphoreType.DMA, pltpu.SemaphoreType.DMA, dma(RELAYED + 2), pltpu.SemaphoreType.DMA, dma(6),
            pltpu.SemaphoreType.DMA, pltpu.SemaphoreType.DMA, pltpu.SemaphoreType.DMA, dma(2),
        ],
        compiler_params=pltpu.CompilerParams(
            collective_id=0, has_side_effects=True, vmem_limit_bytes=66700000
        ),
        name="fused_block",
    )(
        latent.reshape(2, half, width),
        condition,
        context[0],
        context_vector[None, :],
        modulator,
        norm_gain[None, :],
        query_weight,
        key_weight,
        value_weight,
        head_gain[None, :],
        lambdas[None, :],
        context_bias,
        out_weight.reshape(4, wrows, width),
    )
    return result[None]


def choose(axes, *arrays):
    sp_n, tp_n, dp_n = axes
    latent, modulator, query_weight, value_weight = arrays[0], arrays[4], arrays[6], arrays[8]
    lambdas, out_weight, context = arrays[10], arrays[12], arrays[2]
    fits = (
        tp_n == 4
        and dp_n == 2
        and sp_n == 4
        and lambdas.shape[0] == 1
        and query_weight.shape[1] == LANES
        and value_weight.shape[1] == LANES
        and modulator.shape[1] == 3 * latent.shape[2]
        and modulator.shape[0] % LANES == 0
        and context.shape[1] % 8 == 0
        and latent.shape[1] % 32 == 0
        and latent.shape[2] % 512 == 0
        and out_weight.shape[0] % 64 == 0
    )
    return fused(axes, *arrays) if fits else body(*arrays)


def solution(mesh):
    placed = (
        P("dp", ("sp", "tp"), None),
        P("dp", ("sp", "tp")),
        P("dp", "sp", None),
        P(("sp", "tp")),
        P(("sp", "tp"), None),
        P(),
        P(None, "tp"),
        P(None, "tp"),
        P(None, "tp"),
        P(),
        P("tp"),
        P("tp", None),
        P("tp", None),
    )
    axes = (mesh.shape["sp"], mesh.shape["tp"], mesh.shape["dp"])
    return jax.shard_map(
        functools.partial(choose, axes), mesh=mesh, in_specs=placed, out_specs=P("dp", ("sp", "tp"), None), check_vma=False
    )
```
